32 devices in a mesh: sp: 8 (over z, y), tp: 4 (over x, core).
Axes of the slice: x: 2, y: 2, z: 4, core: 2. Of those that a mesh axis runs over, the one named last changes fastest.
Arguments:
- tokens: bfloat16 [2048, 2048], P('sp', 'tp'), may hold values from -6 to 6
- in_gain: float32 [2048], replicated, may hold values from 0.1 to 1.9
- query_down: bfloat16 [2048, 512], replicated, may hold values from -0.125 to 0.125
- latent_down: bfloat16 [2048, 256], replicated, may hold values from -0.125 to 0.125
- rope_down: bfloat16 [2048, 32], replicated, may hold values from -0.125 to 0.125
- query_gain: float32 [512], replicated, may hold values from 0.5 to 12
- latent_gain: float32 [256], replicated, may hold values from 0.5 to 12
- query_nope: bfloat16 [512, 1024], P(None, 'tp'), may hold values from -0.25 to 0.25
- query_rope: bfloat16 [512, 512], P(None, 'tp'), may hold values from -0.25 to 0.25
- key_up: bfloat16 [256, 1024], P(None, 'tp'), may hold values from -0.375 to 0.375
- value_up: bfloat16 [256, 1024], P(None, 'tp'), may hold values from -0.375 to 0.375
- conv_value: bfloat16 [2048, 2048], P(None, 'tp'), may hold values from -0.125 to 0.125
- conv_gate: bfloat16 [2048, 2048], P(None, 'tp'), may hold values from -0.125 to 0.125
- conv_taps: float32 [31, 2048], P(None, 'tp'), may hold values from -1 to 1
- conv_bias: float32 [2048], P('tp'), may hold values from 0.05 to 2.25
- channel_gain: float32 [2048], P('tp'), may hold values from 0.1 to 1.9
- out_attend: bfloat16 [1024, 2048], P('tp'), may hold values from -0.109375 to 0.109375
- out_conv: bfloat16 [2048, 2048], P('tp'), may hold values from -0.109375 to 0.109375
Outputs:
- mixed: bfloat16 [2048, 2048], P('sp', 'tp')
The draws below stay inside these ranges and needn't reach their ends.
All inputs are finite; a program needn't handle non-finite values.
Results may differ from the reference program's by a relative error of at most 0.013.
The reference program's roundings to bfloat16 on the way count: a program that leaves them out, or rounds other values in their place, can miss the bound.
Values may be sent and summed in bfloat16 or wider, within the bound.
A program may use at most 128 MiB of HBM per device.

```python
import math
import jax
import jax.numpy as jnp
from jax import lax

D = 2048
HEADS = 16
NOPE = 64
ROPE = 32
VDIM = 64
QRANK = 512
KVRANK = 256
CONV_CH = 2048
KWIDTH = 31
SEQ = 2048
GROUPS = 4


def draw_query_gain(key, part):
    return jax.random.uniform(key, (QRANK,), jnp.float32, 0.5, 1.5)


def draw_latent_gain(key, part):
    return jax.random.uniform(key, (KVRANK,), jnp.float32, 0.5, 1.5)


def draw_conv_bias(key, part):
    factor = jax.random.uniform(key, (CONV_CH,), jnp.float32, 0.5, 1.5)
    ramp = jnp.arange(CONV_CH).astype(jnp.float32) / (CONV_CH - 1)
    level = 0.1 + 0.9 * ramp
    return level * factor


def level_of(rng, extent, pieces, low, top_value):
    level, own = 1.0, jax.random.fold_in(rng, 6)
    for dim, blocks in pieces:
        draws = jnp.exp(jax.random.uniform(jax.random.fold_in(own, dim), (blocks,), jnp.float32, low / len(pieces), top_value / len(pieces)))
        level = level * jnp.repeat(draws, extent[dim] // blocks).reshape([-1 if axis == dim else 1 for axis in range(len(extent))])
    return level


def normal_values(rng, shape, deviation, most, shards=(), kind=jnp.bfloat16):
    result = deviation * jax.random.normal(rng, shape, jnp.float32)
    if shards:
        result = result * level_of(rng, shape, shards, -0.22, 0.18)
    return jnp.clip(result, -most, most).astype(kind)


def setup_inputs(seed: int = 0) -> dict:
    key_of = jax.random.split(jax.random.key(seed), 19)
    tokens = normal_values(key_of[0], (SEQ, D), 1.0, 6.0, ((0, 8), (1, 4)))
    in_gain = jnp.clip(1.0 + 0.18 * jax.random.normal(key_of[1], (D,), jnp.float32), 0.1, 1.9)
    query_down = normal_values(key_of[2], (D, QRANK), D ** -0.5, 0.125)
    latent_down = normal_values(key_of[3], (D, KVRANK), D ** -0.5, 0.125)
    rope_down = normal_values(key_of[4], (D, ROPE), D ** -0.5, 0.125)
    query_gain = draw_query_gain(jax.random.fold_in(key_of[18], 71), 0)
    latent_gain = draw_latent_gain(jax.random.fold_in(key_of[18], 71), 0)
    query_nope = normal_values(key_of[7], (QRANK, HEADS * NOPE), QRANK ** -0.5, 0.25, ((1, 4),))
    query_rope = normal_values(key_of[8], (QRANK, HEADS * ROPE), QRANK ** -0.5, 0.25, ((1, 4),))
    key_up = normal_values(key_of[9], (KVRANK, HEADS * NOPE), KVRANK ** -0.5, 0.375, ((1, 4),))
    value_up = normal_values(key_of[10], (KVRANK, HEADS * VDIM), KVRANK ** -0.5, 0.375, ((1, 4),))
    conv_value = normal_values(key_of[11], (D, CONV_CH), D ** -0.5, 0.125, ((1, 4),))
    conv_gate = normal_values(key_of[12], (D, CONV_CH), D ** -0.5, 0.125, ((1, 4),))
    conv_taps = normal_values(key_of[13], (KWIDTH, CONV_CH), KWIDTH ** -0.5, 1.0, ((1, 4),), jnp.float32)
    conv_bias = draw_conv_bias(jax.random.fold_in(key_of[18], 71), 0)
    channel_gain = jnp.clip(1.0 + 0.18 * jax.random.normal(key_of[15], (CONV_CH,), jnp.float32), 0.1, 1.9)
    out_attend = normal_values(key_of[16], (HEADS * VDIM, D), (HEADS * VDIM + CONV_CH) ** -0.5, 0.109375, ((0, 4),))
    out_conv = normal_values(key_of[17], (CONV_CH, D), (HEADS * VDIM + CONV_CH) ** -0.5, 0.109375, ((0, 4),))
    return dict(tokens=tokens, in_gain=in_gain, query_down=query_down, latent_down=latent_down, rope_down=rope_down, query_gain=query_gain, latent_gain=latent_gain, query_nope=query_nope, query_rope=query_rope, key_up=key_up, value_up=value_up, conv_value=conv_value, conv_gate=conv_gate, conv_taps=conv_taps, conv_bias=conv_bias, channel_gain=channel_gain, out_attend=out_attend, out_conv=out_conv)


eps_norm = 1e-06
eps_layer = 1e-05
theta = 10000.0

def rms_scale(values, gain):
    return values * lax.rsqrt(lax.optimization_barrier(jnp.mean(values * values, axis=-1, keepdims=True)) + eps_norm) * gain

def rotate(values, positions):
    half = values.shape[-1] // 2
    freqs = theta ** (-jnp.arange(half).astype(jnp.float32) / half)
    angles = positions[..., None] * freqs
    cosine = jnp.cos(angles)
    sine = jnp.sin(angles)
    first = values[..., :half]
    second = values[..., half:]
    return jnp.concatenate([first * cosine - second * sine, second * cosine + first * sine], axis=-1)

def reference(tokens, in_gain, query_down, latent_down, rope_down, query_gain, latent_gain, query_nope, query_rope, key_up, value_up, conv_value, conv_gate, conv_taps, conv_bias, channel_gain, out_attend, out_conv):
    tokens_f = tokens.astype(jnp.float32)
    row_scale = lax.rsqrt(lax.optimization_barrier(jnp.mean(tokens_f * tokens_f, axis=-1, keepdims=True)) + eps_norm)
    scaled = (tokens_f * in_gain).astype(jnp.bfloat16)
    positions = jnp.arange(SEQ).astype(jnp.float32)

    def project(weight):
        return row_scale * jnp.dot(scaled, weight, preferred_element_type=jnp.float32)
    q_latent = rms_scale(project(query_down), query_gain).astype(jnp.bfloat16)
    kv_latent = rms_scale(project(latent_down), latent_gain).astype(jnp.bfloat16)
    rope_key = rotate(project(rope_down), positions).astype(jnp.bfloat16)
    q_nope = jnp.dot(q_latent, query_nope, preferred_element_type=jnp.float32).astype(jnp.bfloat16)
    q_turn = jnp.dot(q_latent, query_rope, preferred_element_type=jnp.float32).reshape(SEQ, HEADS, ROPE)
    q_rope = rotate(q_turn, positions[:, None]).astype(jnp.bfloat16)
    k_nope = jnp.dot(kv_latent, key_up, preferred_element_type=jnp.float32).astype(jnp.bfloat16)
    values = jnp.dot(kv_latent, value_up, preferred_element_type=jnp.float32).astype(jnp.bfloat16)
    key_heads = k_nope.astype(jnp.float32).reshape(SEQ, HEADS, NOPE)
    value_heads = values.astype(jnp.float32).reshape(SEQ, HEADS, VDIM)
    rope_f = rope_key.astype(jnp.float32)
    score_scale = (NOPE + ROPE) ** (-0.5)
    block = math.gcd(SEQ, 256)
    q_blocks = q_nope.reshape(SEQ // block, block, HEADS, NOPE)
    r_blocks = q_rope.reshape(SEQ // block, block, HEADS, ROPE)

    def attend(pair):
        q_part = pair[0].astype(jnp.float32)
        r_part = pair[1].astype(jnp.float32)
        scores = (jnp.einsum('qhd,khd->hqk', q_part, key_heads) + jnp.einsum('qhd,kd->hqk', r_part, rope_f)) * score_scale
        highest = lax.optimization_barrier(jnp.max(scores, axis=-1, keepdims=True))
        weight = jnp.exp(scores - highest)
        total = lax.optimization_barrier(jnp.sum(weight, axis=-1))
        rounded = lax.optimization_barrier(weight.astype(jnp.bfloat16)).astype(jnp.float32)
        summed = jnp.einsum('hqk,khd->qhd', rounded, value_heads)
        return (summed / jnp.transpose(total)[:, :, None]).astype(jnp.bfloat16)
    attended = lax.map(attend, (q_blocks, r_blocks)).reshape(SEQ, HEADS * VDIM)
    glu = (project(conv_value) * jax.nn.sigmoid(project(conv_gate))).astype(jnp.bfloat16)
    half = KWIDTH // 2
    padded = jnp.pad(glu.astype(jnp.float32), ((half, half), (0, 0)))
    conv = jnp.zeros((SEQ, CONV_CH), jnp.float32) + conv_bias
    for tap in range(KWIDTH):
        conv = conv + conv_taps[tap] * padded[tap:tap + SEQ]
    mean = lax.optimization_barrier(jnp.mean(conv, axis=-1, keepdims=True))
    centred = conv - mean
    spread = lax.optimization_barrier(jnp.mean(centred * centred, axis=-1, keepdims=True))
    activated = jax.nn.silu(centred * lax.rsqrt(spread + eps_layer) * channel_gain).astype(jnp.bfloat16)
    head_cols = HEADS * VDIM // GROUPS
    chan_cols = CONV_CH // GROUPS
    mixed = jnp.zeros((SEQ, D), jnp.float32)
    for group in range(GROUPS):
        part_attend = jnp.dot(attended[:, group * head_cols:(group + 1) * head_cols], out_attend[group * head_cols:(group + 1) * head_cols], preferred_element_type=jnp.float32)
        part_conv = jnp.dot(activated[:, group * chan_cols:(group + 1) * chan_cols], out_conv[group * chan_cols:(group + 1) * chan_cols], preferred_element_type=jnp.float32)
        mixed = mixed + (part_attend + part_conv).astype(jnp.bfloat16).astype(jnp.float32)
    return mixed.astype(jnp.bfloat16)
```

```python
import functools

import jax
import jax.numpy as jnp
import numpy as np
from jax import lax
from jax.experimental import pallas as pl
from jax.experimental.pallas import tpu as pltpu
from jax.sharding import PartitionSpec as P

eps_norm = 1e-06
eps_layer = 1e-05
theta = 10000.0
LANES = 128
MESH = pl.DeviceIdType.MESH
bf16 = jnp.bfloat16
f32 = jnp.float32


def dot(a, b):
    return jnp.dot(a, b, preferred_element_type=f32)


def dot_t(a, b):
    return lax.dot_general(a, b, (((1,), (1,)), ((), ())), preferred_element_type=f32)


def body(
    n_sp, n_tp, rope, nope, heads, tchunks, rblocks, kchunk,
    tok, gain, wq, wl, wr, qgain, lgain, wqn, wqr, wku, wvu, wcv, wcg, taps, bias, cgain,
    woa, woc, cos_off, sin_off, cos_base, sin_base, spread_mat,
    out,
    v_tok, v_wq, v_wl, v_wr, v_wqn, v_wqr, v_wku, v_wvu, v_wcv, v_wcg, v_woa, v_woc, v_sp,
    acc_q, acc_l, acc_r, acc_v, acc_g,
    kvr, k_all, v_all, r_all, qf, glu_pad, conv_in, conv_out, stats, act, att,
    cpart, own_part, to_partner, from_partner, to_cross, from_cross,
    w_sem, tx_s, tx_r, tp_s, tp_r, tr_s, tr_r, kx_s, kx_r, ky_s, ky_r,
    h_s, h_r, st_s, st_r, pp_s, pp_r, cc_s, cc_r,
):
    sp, tp = lax.axis_index("sp"), lax.axis_index("tp")
    pairs = n_tp // 2
    pair, core = tp // 2, tp % 2
    partner = pair * 2 + (1 - core)
    rows, dl = tok.shape
    width = n_tp * dl
    kvw = wl.shape[1]
    half = rows // 2
    groups = kvw // rope
    prow = half // groups
    rw = heads * rope
    ch = wcv.shape[1]
    ntap = taps.shape[0]
    pad = glu_pad.shape[0] - rows
    pad = pad // 2

    def rcopy(src, dst, ssem, rsem, to_sp, to_tp):
        return pltpu.make_async_remote_copy(
            src_ref=src, dst_ref=dst, send_sem=ssem, recv_sem=rsem,
            device_id=(to_sp, to_tp), device_id_type=MESH)

    loads = {}
    for i, (name, src, dst) in enumerate([
        ("tok", tok, v_tok.at[tp]), ("wl", wl, v_wl), ("wr", wr, v_wr), ("wq", wq, v_wq),
        ("wcv", wcv, v_wcv), ("wcg", wcg, v_wcg), ("wqn", wqn, v_wqn), ("wqr", wqr, v_wqr),
        ("wku", wku, v_wku), ("wvu", wvu, v_wvu), ("sp", spread_mat, v_sp),
        ("woc", woc, v_woc), ("woa", woa, v_woa),
    ]):
        loads[name] = pltpu.make_async_copy(src, dst, w_sem.at[i])
        loads[name].start()

    barrier = pltpu.get_barrier_semaphore()
    for d in range(1, n_tp):
        pl.semaphore_signal(barrier, inc=1, device_id=(sp, (tp + d) % n_tp), device_id_type=MESH)
    for d in range(1, n_sp):
        pl.semaphore_signal(barrier, inc=1, device_id=((sp + d) % n_sp, tp), device_id_type=MESH)
    pl.semaphore_wait(barrier, n_tp - 1 + n_sp - 1)

    tr = rows // tchunks
    sends = []
    for j in range(1, pairs):
        for r in range(tchunks):
            part = pl.ds(r * tr, tr)
            c = rcopy(tok.at[part], v_tok.at[tp, part], tx_s.at[j, r], tx_r.at[j, r],
                      sp, ((pair + j) % pairs) * 2 + core)
            c.start()
            sends.append(c)
    to_p = rcopy(tok, v_tok.at[tp], tp_s, tp_r, sp, partner)
    to_p.start()
    sends.append(to_p)

    def shard(t):
        x = v_tok[t].astype(f32)
        g = gain[:, pl.ds(pl.multiple_of(t * dl, LANES), dl)]
        return (x * g).astype(bf16), jnp.sum(x * x, axis=1, keepdims=True)

    def wrows(ref, t):
        return ref[pl.ds(pl.multiple_of(t * dl, LANES), dl), :]

    everything = ((acc_l, v_wl), (acc_r, v_wr), (acc_q, v_wq), (acc_v, v_wcv), (acc_g, v_wcg))
    loads["tok"].wait()
    xs, sq = shard(tp)
    for name in ("wl", "wr", "wq", "wcv", "wcg"):
        loads[name].wait()
    for acc, w in everything:
        acc[...] = dot(xs, wrows(w, tp))
    to_p.wait_recv()
    xs, s = shard(partner)
    sq = sq + s
    for acc, w in everything:
        acc[...] += dot(xs, wrows(w, partner))
    for j in range(1, pairs):
        src_t = ((pair + pairs - j) % pairs) * 2 + core
        for r in range(tchunks):
            part = pl.ds(r * tr, tr)
            rcopy(tok.at[part], v_tok.at[src_t, part], tx_s.at[j, r], tx_r.at[j, r], sp, partner).wait_recv()
            c = rcopy(v_tok.at[src_t, part], v_tok.at[src_t, part], tr_s.at[j, r], tr_r.at[j, r], sp, partner)
            c.start()
            sends.append(c)
    rest = []
    for j in range(1, pairs):
        base = ((pair + pairs - j) % pairs) * 2
        xs, s = shard(base + core)
        sq = sq + s
        acc_l[...] += dot(xs, wrows(v_wl, base + core))
        acc_r[...] += dot(xs, wrows(v_wr, base + core))
        rest.append((xs, base + core))
    for j in range(1, pairs):
        base = ((pair + pairs - j) % pairs) * 2
        other = base + (1 - core)
        for r in range(tchunks):
            part = pl.ds(r * tr, tr)
            rcopy(v_tok.at[other, part], v_tok.at[other, part], tr_s.at[j, r], tr_r.at[j, r], sp, partner).wait_recv()
        xs, s = shard(other)
        sq = sq + s
        acc_l[...] += dot(xs, wrows(v_wl, other))
        acc_r[...] += dot(xs, wrows(v_wr, other))
        rest.append((xs, other))
    row_scale = lax.rsqrt(sq * (1.0 / width) + eps_norm)

    def rms(v, g):
        return v * lax.rsqrt(jnp.mean(v * v, axis=-1, keepdims=True) + eps_norm) * g

    cb, sb = cos_base[pl.ds(sp, 1), :], sin_base[pl.ds(sp, 1), :]
    co, so = cos_off[...], sin_off[...]
    cosine = cb * co - sb * so
    sine = sb * co + cb * so

    def turn(v, w):
        lane = lax.broadcasted_iota(jnp.int32, v.shape, 1)
        first = None
        for g in range(w // rope):
            m = (lane >= g * rope) & (lane < g * rope + rope // 2)
            first = m if first is None else first | m
        up = pltpu.roll(v, w - rope // 2, axis=1)
        down = pltpu.roll(v, rope // 2, axis=1)
        return v * cosine[:, :w] + jnp.where(first, -up, down) * sine[:, :w]

    kv = rms(row_scale * acc_l[...], lgain[...]).astype(bf16)
    rk = row_scale * acc_r[...]
    rk = turn(jnp.concatenate([rk] * groups, axis=1), kvw)
    lane_p = lax.broadcasted_iota(jnp.int32, (prow, kvw), 1)
    for hf in range(2):
        kvr[sp, hf, 0:half, :] = kv[hf * half:(hf + 1) * half]
        packed = jnp.zeros((prow, kvw), f32)
        for g in range(groups):
            piece = rk[hf * half + g * prow: hf * half + (g + 1) * prow]
            packed = jnp.where((lane_p >= g * rope) & (lane_p < (g + 1) * rope), piece, packed)
        kvr[sp, hf, half:half + prow, :] = packed.astype(bf16)
    for d in range(1, n_sp):
        c = rcopy(kvr.at[sp, core], kvr.at[sp, core], kx_s.at[d], kx_r.at[d], (sp + d) % n_sp, tp)
        c.start()
        sends.append(c)

    for xs, t in rest:
        acc_v[...] += dot(xs, wrows(v_wcv, t))
        acc_g[...] += dot(xs, wrows(v_wcg, t))
    glu = (row_scale * acc_v[...] * jax.nn.sigmoid(row_scale * acc_g[...])).astype(bf16)
    glu_pad[pad:pad + rows, :] = glu
    zeros_halo = jnp.zeros((pad, ch), bf16)

    def halo(up):
        if up:
            return rcopy(glu_pad.at[pl.ds(rows, pad)], glu_pad.at[pl.ds(0, pad)],
                         h_s.at[0], h_r.at[0], (sp + 1) % n_sp, tp)
        return rcopy(glu_pad.at[pl.ds(pad, pad)], glu_pad.at[pl.ds(pad + rows, pad)],
                     h_s.at[1], h_r.at[1], (sp + n_sp - 1) % n_sp, tp)

    @pl.when(sp < n_sp - 1)
    def _():
        halo(True).start()

    @pl.when(sp > 0)
    def _():
        halo(False).start()

    @pl.when(sp == 0)
    def _():
        glu_pad[0:pad, :] = zeros_halo

    @pl.when(sp == n_sp - 1)
    def _():
        glu_pad[pad + rows:pad + rows + pad, :] = zeros_halo

    for xs, t in rest:
        acc_q[...] += dot(xs, wrows(v_wq, t))
    ql = rms(row_scale * acc_q[...], qgain[...]).astype(bf16)
    for name in ("wqn", "wqr"):
        loads[name].wait()
    qn = dot(ql, v_wqn[...])
    qr = turn(dot(ql, v_wqr[...]), rw)
    per = LANES // nope
    lane_n = lax.broadcasted_iota(jnp.int32, (rows, LANES), 1)
    lane_r = lax.broadcasted_iota(jnp.int32, (rows, rw), 1)
    for h in range(heads):
        blk, off = h // per, (h % per) * nope
        qf[h, :, 0:LANES] = jnp.where(
            (lane_n >= off) & (lane_n < off + nope), qn[:, blk * LANES:(blk + 1) * LANES], 0.0).astype(bf16)
        qf[h, :, LANES:LANES + rw] = jnp.where(
            (lane_r >= h * rope) & (lane_r < (h + 1) * rope), qr, 0.0).astype(bf16)

    def relay(d, start):
        src = (sp + n_sp - d) % n_sp
        if start:
            rcopy(kvr.at[src, core], kvr.at[src, core], kx_s.at[d], kx_r.at[d], sp, partner).wait_recv()
            c = rcopy(kvr.at[src, core], kvr.at[src, core], ky_s.at[d], ky_r.at[d], sp, partner)
            c.start()
            sends.append(c)
        else:
            other = kvr.at[src, 1 - core]
            rcopy(other, other, ky_s.at[d], ky_r.at[d], sp, partner).wait_recv()

    @pl.when(sp < n_sp - 1)
    def _():
        halo(True).wait_send()
        halo(False).wait_recv()

    @pl.when(sp > 0)
    def _():
        halo(False).wait_send()
        halo(True).wait_recv()

    conv_in[...] = glu_pad[...].astype(f32)
    rb = rows // 2
    first_off = pad - ntap // 2
    s1, s2 = [], []
    for b in range(2):
        t1 = jnp.zeros((rb, LANES), f32)
        t2 = jnp.zeros((rb, LANES), f32)
        for l in range(ch // LANES):
            cols = slice(l * LANES, (l + 1) * LANES)
            x = conv_in[b * rb:b * rb + rb + 2 * pad, cols]
            n = rb + 2 * pad
            acc = jnp.zeros((rb, LANES), f32) + bias[:, cols]
            for res in range(8):
                xr = x if res == 0 else pltpu.roll(x, n - res, axis=0)
                for k in range(ntap):
                    if (k + first_off) % 8 == res:
                        o = k + first_off - res
                        acc = acc + taps[k:k + 1, cols] * xr[o:o + rb]
            conv_out[b * rb:(b + 1) * rb, cols] = acc
            t1 = t1 + acc
            t2 = t2 + acc * acc
        s1.append(jnp.sum(t1, axis=1, keepdims=True))
        s2.append(jnp.sum(t2, axis=1, keepdims=True))
    s1 = jnp.concatenate(s1, axis=0)
    s2 = jnp.concatenate(s2, axis=0)
    lane_s = lax.broadcasted_iota(jnp.int32, (rows, LANES), 1)
    stats[tp] = jnp.transpose(jnp.where(lane_s == 0, s1, jnp.where(lane_s == 1, s2, 0.0)))[0:8]
    for d in range(1, n_tp):
        c = rcopy(stats.at[tp], stats.at[tp], st_s.at[d], st_r.at[d], sp, (tp + d) % n_tp)
        c.start()
        sends.append(c)
    order = list(range(1, n_sp))
    for d in order:
        relay(d, True)

    for d in range(1, n_tp):
        src = (tp + n_tp - d) % n_tp
        rcopy(stats.at[src], stats.at[src], st_s.at[d], st_r.at[d], sp, partner).wait_recv()
    tot = stats[0]
    for t in range(1, n_tp):
        tot = tot + stats[t]
    tot = jnp.transpose(jnp.concatenate([tot, jnp.zeros((LANES - 8, rows), f32)], axis=0))
    mean = tot[:, 0:1] * (1.0 / (ch * n_tp))
    var = tot[:, 1:2] * (1.0 / (ch * n_tp)) - mean * mean
    y = (conv_out[...] - mean) * lax.rsqrt(var + eps_layer) * cgain[...]
    act[...] = (y * jax.nn.sigmoid(y)).astype(bf16)
    loads["woc"].wait()
    cpart[...] = dot(act[...], v_woc[...])

    for d in order:
        relay(d, False)

    for name in ("wku", "wvu", "sp"):
        loads[name].wait()

    def expand(s, _):
        for hf in range(2):
            lat = kvr[s, hf, 0:half, :]
            at = pl.ds(pl.multiple_of(s * rows, rows) + hf * half, half)
            k_all[at, :] = dot(lat, v_wku[...]).astype(bf16)
            v_all[at, :] = dot(lat, v_wvu[...]).astype(bf16)
            u = dot(kvr[s, hf, half:half + prow, :], v_sp[...]).astype(bf16)
            for g in range(groups):
                r_all[pl.ds(pl.multiple_of(s * rows, rows) + hf * half + g * prow, prow), :] = u[:, g * rw:(g + 1) * rw]
        return 0

    lax.fori_loop(0, n_sp, expand, 0)

    keys = n_sp * rows
    nk = keys // kchunk
    qb = rows // rblocks
    vw = v_all.shape[1]
    vdim = vw // heads
    scale2 = float((nope + rope) ** -0.5 * np.log2(np.e))
    lane_v = lax.broadcasted_iota(jnp.int32, (qb, vw), 1)

    def attend(b, hs, result):
        for h in hs:
            blk = h // per
            q = qf[h, b * qb:(b + 1) * qb, :]

            def scores(at):
                k = jnp.concatenate([k_all[at, blk * LANES:(blk + 1) * LANES], r_all[at, :]], axis=1)
                return dot_t(q, k)

            if nk == 1:
                at = slice(0, keys)
                s = scores(at)
                m = jnp.max(s, axis=1, keepdims=True)
                w = jnp.exp2((s - m) * scale2)
                total = jnp.sum(w, axis=1, keepdims=True)
                o = dot(w.astype(bf16), v_all[at, :])
            else:
                def step(i, carry):
                    m, total, o = carry
                    at = pl.ds(pl.multiple_of(i * kchunk, kchunk), kchunk)
                    s = scores(at)
                    nm = jnp.maximum(m, jnp.max(s, axis=1, keepdims=True))
                    f = jnp.exp2((m - nm) * scale2)
                    w = jnp.exp2((s - nm) * scale2)
                    return (nm, total * f + jnp.sum(w, axis=1, keepdims=True),
                            o * f + dot(w.astype(bf16), v_all[at, :]))
                m, total, o = lax.fori_loop(0, nk, step, (
                    jnp.full((qb, 1), -jnp.inf, f32), jnp.zeros((qb, 1), f32), jnp.zeros((qb, vw), f32)))
            mask = (lane_v >= h * vdim) & (lane_v < (h + 1) * vdim)
            result = jnp.where(mask, o / total, result)
        return result

    def partial(b, t, a):
        cols = pl.ds(pl.multiple_of(t * dl, LANES), dl)
        return (dot(a, v_woa[:, cols]) + cpart[b * qb:(b + 1) * qb, cols]).astype(bf16)

    def pcopy(b, j):
        return rcopy(to_partner.at[b, j], from_partner.at[b, j], pp_s.at[b, j], pp_r.at[b, j], sp, partner)

    def ccopy(b, j):
        return rcopy(to_cross.at[b, j], from_cross.at[b, j], cc_s.at[b, j], cc_r.at[b, j],
                     sp, ((pair + j) % pairs) * 2 + core)

    def project(b, a):
        for j in list(range(1, pairs)) + [0]:
            t = ((pair + j) % pairs) * 2
            to_partner[b, j] = partial(b, t + (1 - core), a)
            pcopy(b, j).start()
        for j in range(pairs):
            t = ((pair + j) % pairs) * 2
            own_part[b, j] = partial(b, t + core, a)

    def cross(b):
        for j in range(1, pairs):
            pcopy(b, j).wait_recv()
            to_cross[b, j] = (own_part[b, j].astype(f32) + from_partner[b, j].astype(f32)).astype(bf16)
            ccopy(b, j).start()

    zero = jnp.zeros((qb, vw), f32)
    loads["woa"].wait()
    for b in range(rblocks):
        a = attend(b, range(heads // 2), zero)
        if b:
            cross(b - 1)
        a = attend(b, range(heads // 2, heads), a)
        project(b, a.astype(bf16))
    cross(rblocks - 1)
    for b in range(rblocks):
        pcopy(b, 0).wait_recv()
        total = own_part[b, 0].astype(f32) + from_partner[b, 0].astype(f32)
        for j in range(1, pairs):
            ccopy(b, j).wait_recv()
            total = total + from_cross[b, j].astype(f32)
        out[b * qb:(b + 1) * qb, :] = total.astype(bf16)
    for b in range(rblocks):
        for j in range(pairs):
            pcopy(b, j).wait_send()
        for j in range(1, pairs):
            ccopy(b, j).wait_send()
    for c in sends:
        c.wait_send()


def per_device(n_sp, n_tp, *args):
    (tokens, in_gain, query_down, latent_down, rope_down, query_gain, latent_gain, query_nope,
     query_rope, key_up, value_up, conv_value, conv_gate, conv_taps, conv_bias, channel_gain,
     out_attend, out_conv) = args
    rows, dl = tokens.shape
    rope = rope_down.shape[1]
    heads = query_rope.shape[1] // rope
    nope = query_nope.shape[1] // heads
    kvw, qw = latent_down.shape[1], query_down.shape[1]
    ch = conv_value.shape[1]
    groups, half = kvw // rope, rows // 2
    prow = half // groups
    rw = heads * rope
    pairs = n_tp // 2
    tchunks, rblocks = 4, 2
    keys = n_sp * rows
    kchunk = min(keys, 2048)
    qb = rows // rblocks
    pad = -(-(conv_taps.shape[0] // 2) // 16) * 16
    freqs = np.float64(theta) ** (-np.arange(rope // 2) / (rope // 2))
    freqs = np.tile(freqs, 2 * groups)[None, :]
    off = np.arange(rows)[:, None] * freqs
    base = (np.arange(n_sp) * rows)[:, None] * freqs
    tables = [np.cos(off), np.sin(off), np.cos(base), np.sin(base)]
    tables = [jnp.asarray(t.astype(np.float32)) for t in tables]
    l = np.arange(kvw)[:, None]
    m = np.arange(groups * rw)[None, :]
    spread_mat = jnp.asarray(((l // rope == m // rw) & (l % rope == m % rope)).astype(np.float32), bf16)
    row = lambda v: v.reshape(1, -1)
    ins = (tokens, row(in_gain), query_down, latent_down, rope_down, row(query_gain), row(latent_gain),
           query_nope, query_rope, key_up, value_up, conv_value, conv_gate, conv_taps, row(conv_bias),
           row(channel_gain), out_attend, out_conv, *tables, spread_mat)
    A, V = pl.BlockSpec(memory_space=pl.ANY), pl.BlockSpec(memory_space=pltpu.VMEM)
    specs = [A, V, A, A, A, V, V, A, A, A, A, A, A, V, V, V, A, A, V, V, V, V, A]
    vm = lambda a: pltpu.VMEM(a.shape, a.dtype)
    D = lambda *s: pltpu.SemaphoreType.DMA(s)
    scratch = [
        pltpu.VMEM((n_tp, rows, dl), bf16), vm(query_down), vm(latent_down), vm(rope_down),
        vm(query_nope), vm(query_rope), vm(key_up), vm(value_up), vm(conv_value), vm(conv_gate),
        vm(out_attend), vm(out_conv), vm(spread_mat),
        pltpu.VMEM((rows, qw), f32), pltpu.VMEM((rows, kvw), f32), pltpu.VMEM((rows, rope), f32),
        pltpu.VMEM((rows, ch), f32), pltpu.VMEM((rows, ch), f32),
        pltpu.VMEM((n_sp, 2, half + prow, kvw), bf16),
        pltpu.VMEM((keys, key_up.shape[1]), bf16), pltpu.VMEM((keys, value_up.shape[1]), bf16),
        pltpu.VMEM((keys, rw), bf16), pltpu.VMEM((heads, rows, LANES + rw), bf16),
        pltpu.VMEM((rows + 2 * pad, ch), bf16), pltpu.VMEM((rows + 2 * pad, ch), f32),
        pltpu.VMEM((rows, ch), f32), pltpu.VMEM((n_tp, 8, rows), f32), pltpu.VMEM((rows, ch), bf16),
        pltpu.VMEM((8, LANES), f32),
        pltpu.VMEM((rows, n_tp * dl), f32),
        pltpu.VMEM((rblocks, pairs, qb, dl), bf16), pltpu.VMEM((rblocks, pairs, qb, dl), bf16),
        pltpu.VMEM((rblocks, pairs, qb, dl), bf16), pltpu.VMEM((rblocks, pairs, qb, dl), bf16),
        pltpu.VMEM((rblocks, pairs, qb, dl), bf16),
        D(13), D(pairs, tchunks), D(pairs, tchunks), pltpu.SemaphoreType.DMA, pltpu.SemaphoreType.DMA,
        D(pairs, tchunks), D(pairs, tchunks), D(n_sp), D(n_sp), D(n_sp), D(n_sp),
        D(2), D(2), D(n_tp), D(n_tp), D(rblocks, pairs), D(rblocks, pairs),
        D(rblocks, pairs), D(rblocks, pairs),
    ]
    return pl.pallas_call(
        functools.partial(body, n_sp, n_tp, rope, nope, heads, tchunks, rblocks, kchunk),
        out_shape=jax.ShapeDtypeStruct((rows, dl), bf16),
        in_specs=specs,
        out_specs=V,
        scratch_shapes=scratch,
        compiler_params=pltpu.CompilerParams(
            collective_id=0, has_side_effects=True, vmem_limit_bytes=60 * 1024 * 1024),
        name="layer",
    )(*ins)


def solution(mesh):
    in_specs = (
        P("sp", "tp"), P(), P(), P(), P(), P(), P(), P(None, "tp"), P(None, "tp"), P(None, "tp"),
        P(None, "tp"), P(None, "tp"), P(None, "tp"), P(None, "tp"), P("tp"), P("tp"),
        P("tp", None), P("tp", None),
    )
    return jax.shard_map(
        functools.partial(per_device, mesh.shape["sp"], mesh.shape["tp"]),
        mesh=mesh, in_specs=in_specs, out_specs=P("sp", "tp"), check_vma=False)
```

```python
import functools

import jax
import jax.numpy as jnp
import numpy as np
from jax import lax
from jax.experimental import pallas as pl
from jax.experimental.pallas import tpu as pltpu
from jax.sharding import PartitionSpec as P

eps_norm = 1e-06
eps_layer = 1e-05
theta = 10000.0
LANES = 128
MESH = pl.DeviceIdType.MESH
bf16 = jnp.bfloat16
f32 = jnp.float32


def dot(a, b):
    return jnp.dot(a, b, preferred_element_type=f32)


def dot_t(a, b):
    return lax.dot_general(a, b, (((1,), (1,)), ((), ())), preferred_element_type=f32)


def body(
    n_sp, n_tp, rope, nope, heads, tchunks, rblocks, kchunk,
    tok, gain_in, wq, wl, wr, qgain_in, lgain_in, wqn, wqr, wku, wvu, wcv, wcg, taps_in, bias_in,
    cgain_in, woa, woc, cos_off_in, sin_off_in, cos_base_in, sin_base_in, spread_mat,
    out,
    v_tok, v_wq, v_wl, v_wr, v_wqn, v_wqr, v_wku, v_wvu, v_wcv, v_wcg, v_woa, v_woc, v_sp,
    gain, qgain, lgain, taps, bias, cgain, cos_off, sin_off, cos_base, sin_base,
    acc_q, acc_l, acc_r, acc_v, acc_g,
    kvr, k_all, v_all, r_all, qf, glu_pad, conv_in, conv_out, stats, act,
    cpart, own_part, to_partner, from_partner, to_cross, from_cross, result,
    w_sem, tx_s, tx_r, tp_s, tp_r, tr_s, tr_r, ku_s, kd_s, kz_s, kx_r, ky_s, ky_r,
    h_s, h_r, st_s, st_r, pp_s, pp_r, cc_s, cc_r, out_s,
):
    sp, tp = lax.axis_index("sp"), lax.axis_index("tp")
    pairs = n_tp // 2
    pair, core = tp // 2, tp % 2
    partner = pair * 2 + (1 - core)
    rows, dl = tok.shape
    width = n_tp * dl
    kvw = wl.shape[1]
    half = rows // 2
    groups = kvw // rope
    prow = half // groups
    rw = heads * rope
    ch = wcv.shape[1]
    ntap = taps.shape[0]
    pad = glu_pad.shape[0] - rows
    pad = pad // 2

    def rcopy(src, dst, ssem, rsem, to_sp, to_tp):
        return pltpu.make_async_remote_copy(
            src_ref=src, dst_ref=dst, send_sem=ssem, recv_sem=rsem,
            device_id=(to_sp, to_tp), device_id_type=MESH)

    loads = {}
    for i, (name, src, dst) in enumerate([
        ("tok", tok, v_tok.at[tp]), ("gain", gain_in, gain), ("wl", wl, v_wl), ("wr", wr, v_wr), ("wq", wq, v_wq),
        ("wcv", wcv, v_wcv), ("wcg", wcg, v_wcg), ("wqn", wqn, v_wqn), ("wqr", wqr, v_wqr),
        ("wku", wku, v_wku), ("wvu", wvu, v_wvu), ("lgain", lgain_in, lgain), ("qgain", qgain_in, qgain),
        ("co", cos_off_in, cos_off), ("so", sin_off_in, sin_off), ("cb", cos_base_in, cos_base),
        ("sb", sin_base_in, sin_base), ("taps", taps_in, taps), ("bias", bias_in, bias),
        ("cgain", cgain_in, cgain), ("sp", spread_mat, v_sp),
        ("woc", woc, v_woc), ("woa", woa, v_woa),
    ]):
        loads[name] = pltpu.make_async_copy(src, dst, w_sem.at[i])
        loads[name].start()

    barrier = pltpu.get_barrier_semaphore()
    for d in range(1, n_tp):
        pl.semaphore_signal(barrier, inc=1, device_id=(sp, (tp + d) % n_tp), device_id_type=MESH)
    for d in (1, 2):
        for ok, to in ((sp + d < n_sp, (sp + d) % n_sp), (sp >= d, (sp + n_sp - d) % n_sp)):
            @pl.when(ok)
            def _():
                pl.semaphore_signal(barrier, inc=1, device_id=(to, tp), device_id_type=MESH)
    near = jnp.minimum(n_sp - 1 - sp, 2) + jnp.minimum(sp, 2)
    pl.semaphore_wait(barrier, n_tp - 1 + near)

    tr = rows // tchunks
    sends = []
    for j in range(1, pairs):
        for r in range(tchunks):
            part = pl.ds(r * tr, tr)
            c = rcopy(tok.at[part], v_tok.at[tp, part], tx_s.at[j, r], tx_r.at[j, r],
                      sp, ((pair + j) % pairs) * 2 + core)
            c.start()
            sends.append(c)
    to_p = rcopy(tok, v_tok.at[tp], tp_s, tp_r, sp, partner)
    to_p.start()
    sends.append(to_p)

    def shard(t):
        x = v_tok[t].astype(f32)
        g = gain[:, pl.ds(pl.multiple_of(t * dl, LANES), dl)]
        return (x * g).astype(bf16), jnp.sum(x * x, axis=1, keepdims=True)

    def wrows(ref, t):
        return ref[pl.ds(pl.multiple_of(t * dl, LANES), dl), :]

    def rope_rows(xs, t):
        return dot_t(xs, v_wr[:, pl.ds(pl.multiple_of(t * dl, LANES), dl)])

    everything = ((acc_l, v_wl), (acc_q, v_wq), (acc_v, v_wcv), (acc_g, v_wcg))
    loads["tok"].wait()
    loads["gain"].wait()
    xs, sq = shard(tp)
    for name in ("wl", "wr", "wq", "wcv", "wcg"):
        loads[name].wait()
    for acc, w in everything:
        acc[...] = dot(xs, wrows(w, tp))
    acc_r[...] = rope_rows(xs, tp)
    for name in ("lgain", "qgain", "co", "so", "cb", "sb", "taps", "bias", "cgain"):
        loads[name].wait()
    to_p.wait_recv()
    xs, s = shard(partner)
    sq = sq + s
    for acc, w in everything:
        acc[...] += dot(xs, wrows(w, partner))
    acc_r[...] += rope_rows(xs, partner)
    for j in range(1, pairs):
        src_t = ((pair + pairs - j) % pairs) * 2 + core
        for r in range(tchunks):
            part = pl.ds(r * tr, tr)
            rcopy(tok.at[part], v_tok.at[src_t, part], tx_s.at[j, r], tx_r.at[j, r], sp, partner).wait_recv()
            c = rcopy(v_tok.at[src_t, part], v_tok.at[src_t, part], tr_s.at[j, r], tr_r.at[j, r], sp, partner)
            c.start()
            sends.append(c)
    rest = []
    for j in range(1, pairs):
        base = ((pair + pairs - j) % pairs) * 2
        xs, s = shard(base + core)
        sq = sq + s
        acc_l[...] += dot(xs, wrows(v_wl, base + core))
        acc_r[...] += rope_rows(xs, base + core)
        rest.append((xs, base + core))
    for j in range(1, pairs):
        base = ((pair + pairs - j) % pairs) * 2
        other = base + (1 - core)
        for r in range(tchunks):
            part = pl.ds(r * tr, tr)
            rcopy(v_tok.at[other, part], v_tok.at[other, part], tr_s.at[j, r], tr_r.at[j, r], sp, partner).wait_recv()
        xs, s = shard(other)
        sq = sq + s
        acc_l[...] += dot(xs, wrows(v_wl, other))
        acc_r[...] += rope_rows(xs, other)
        rest.append((xs, other))
    row_scale = lax.rsqrt(sq * (1.0 / width) + eps_norm)

    def rms(v, g):
        return v * lax.rsqrt(jnp.mean(v * v, axis=-1, keepdims=True) + eps_norm) * g

    cb, sb = cos_base[pl.ds(sp, 1), :], sin_base[pl.ds(sp, 1), :]
    co, so = cos_off[...], sin_off[...]
    cosine = cb * co - sb * so
    sine = sb * co + cb * so

    def turn(v, w):
        lane = lax.broadcasted_iota(jnp.int32, v.shape, 1)
        first = None
        for g in range(w // rope):
            m = (lane >= g * rope) & (lane < g * rope + rope // 2)
            first = m if first is None else first | m
        up = pltpu.roll(v, w - rope // 2, axis=1)
        down = pltpu.roll(v, rope // 2, axis=1)
        return v * cosine[:, :w] + jnp.where(first, -up, down) * sine[:, :w]

    for xs, t in rest:
        acc_v[...] += dot(xs, wrows(v_wcv, t))
        acc_g[...] += dot(xs, wrows(v_wcg, t))
    glu = (row_scale * acc_v[...] * jax.nn.sigmoid(row_scale * acc_g[...])).astype(bf16)
    glu_pad[pad:pad + rows, :] = glu
    zeros_halo = jnp.zeros((pad, ch), bf16)

    def halo(up):
        if up:
            return rcopy(glu_pad.at[pl.ds(rows, pad)], glu_pad.at[pl.ds(0, pad)],
                         h_s.at[0], h_r.at[0], (sp + 1) % n_sp, tp)
        return rcopy(glu_pad.at[pl.ds(pad, pad)], glu_pad.at[pl.ds(pad + rows, pad)],
                     h_s.at[1], h_r.at[1], (sp + n_sp - 1) % n_sp, tp)

    @pl.when(sp < n_sp - 1)
    def _():
        halo(True).start()

    @pl.when(sp > 0)
    def _():
        halo(False).start()

    @pl.when(sp == 0)
    def _():
        glu_pad[0:pad, :] = zeros_halo

    @pl.when(sp == n_sp - 1)
    def _():
        glu_pad[pad + rows:pad + rows + pad, :] = zeros_halo

    kv = rms(row_scale * acc_l[...], lgain[...]).astype(bf16)
    rk = row_scale * acc_r[...]
    rk = turn(jnp.concatenate([rk] * groups, axis=1), kvw)
    lane_p = lax.broadcasted_iota(jnp.int32, (prow, kvw), 1)
    for hf in range(2):
        kvr[sp, hf, 0:half, :] = kv[hf * half:(hf + 1) * half]
        packed = jnp.zeros((prow, kvw), f32)
        for g in range(groups):
            piece = rk[hf * half + g * prow: hf * half + (g + 1) * prow]
            packed = jnp.where((lane_p >= g * rope) & (lane_p < (g + 1) * rope), piece, packed)
        kvr[sp, hf, half:half + prow, :] = packed.astype(bf16)
    line, place, side = n_sp // 2, sp // 2, sp % 2

    def block(src, sems, to_sp, to_tp, recv, hf=core):
        ref = kvr.at[src, hf]
        return rcopy(ref, ref, sems.at[src], recv.at[src], to_sp, to_tp)

    def when(cond, f):
        @pl.when(cond)
        def _():
            f()

    def passes(src, mode):
        act_on = lambda c: getattr(c, mode)()
        act_on(block(src, kz_s, place * 2 + 1 - side, tp, kx_r))

    def to_partner_core(src, mode):
        getattr(block(src, ky_s, sp, partner, ky_r), mode)()

    def up(src, mode):
        when(place < line - 1, lambda: getattr(block(src, ku_s, (sp + 2) % n_sp, tp, kx_r), mode)())

    def down(src, mode):
        when(place > 0, lambda: getattr(block(src, kd_s, (sp + n_sp - 2) % n_sp, tp, kx_r), mode)())

    def arrived(src):
        block(src, kz_s, sp, partner, kx_r).wait_recv()

    def spread_step(k, mode):
        go = mode == "start"
        if k == 0:
            up(sp, mode)
            down(sp, mode)
            passes(sp, mode)
            return

        def below():
            src = sp - 2 * k
            if go:
                arrived(src)
            up(src, mode)
            passes(src, mode)
            to_partner_core(src, mode)

        def above():
            src = sp + 2 * k
            if go:
                arrived(src)
            down(src, mode)
            passes(src, mode)
            to_partner_core(src, mode)

        when(place >= k, below)
        when(place + k < line, above)

    def other_side(k, mode):
        mine = place * 2 + 1 - side

        def one(src):
            if mode == "start":
                arrived(src)
            to_partner_core(src, mode)

        if k == 0:
            one(mine)
            return
        when(place >= k, lambda: one(mine - 2 * k))
        when(place + k < line, lambda: one(mine + 2 * k))

    spread_step(0, "start")

    for xs, t in rest:
        acc_q[...] += dot(xs, wrows(v_wq, t))
    ql = rms(row_scale * acc_q[...], qgain[...]).astype(bf16)
    for name in ("wqn", "wqr"):
        loads[name].wait()
    qn = dot(ql, v_wqn[...])
    qr = turn(dot(ql, v_wqr[...]), rw)
    per = LANES // nope
    lane_n = lax.broadcasted_iota(jnp.int32, (rows, LANES), 1)
    lane_r = lax.broadcasted_iota(jnp.int32, (rows, rw), 1)
    for h in range(heads):
        blk, off = h // per, (h % per) * nope
        qf[h, :, 0:LANES] = jnp.where(
            (lane_n >= off) & (lane_n < off + nope), qn[:, blk * LANES:(blk + 1) * LANES], 0.0).astype(bf16)
        qf[h, :, LANES:LANES + rw] = jnp.where(
            (lane_r >= h * rope) & (lane_r < (h + 1) * rope), qr, 0.0).astype(bf16)

    @pl.when(sp < n_sp - 1)
    def _():
        halo(True).wait_send()
        halo(False).wait_recv()

    @pl.when(sp > 0)
    def _():
        halo(False).wait_send()
        halo(True).wait_recv()

    conv_in[...] = glu_pad[...].astype(f32)
    rb = rows // 2
    first_off = pad - ntap // 2
    s1, s2 = [], []
    for b in range(2):
        t1 = jnp.zeros((rb, LANES), f32)
        t2 = jnp.zeros((rb, LANES), f32)
        for l in range(ch // LANES):
            cols = slice(l * LANES, (l + 1) * LANES)
            x = conv_in[b * rb:b * rb + rb + 2 * pad, cols]
            n = rb + 2 * pad
            acc = jnp.zeros((rb, LANES), f32) + bias[:, cols]
            for res in range(8):
                xr = x if res == 0 else pltpu.roll(x, n - res, axis=0)
                for k in range(ntap):
                    if (k + first_off) % 8 == res:
                        o = k + first_off - res
                        acc = acc + taps[k:k + 1, cols] * xr[o:o + rb]
            conv_out[b * rb:(b + 1) * rb, cols] = acc
            t1 = t1 + acc
            t2 = t2 + acc * acc
        s1.append(jnp.sum(t1, axis=1, keepdims=True))
        s2.append(jnp.sum(t2, axis=1, keepdims=True))
    s1 = jnp.concatenate(s1, axis=0)
    s2 = jnp.concatenate(s2, axis=0)
    lane_s = lax.broadcasted_iota(jnp.int32, (rows, LANES), 1)
    stats[tp] = jnp.transpose(jnp.where(lane_s == 0, s1, jnp.where(lane_s == 1, s2, 0.0)))[0:8]
    for d in range(1, n_tp):
        c = rcopy(stats.at[tp], stats.at[tp], st_s.at[d], st_r.at[d], sp, (tp + d) % n_tp)
        c.start()
        sends.append(c)
    spread_step(1, "start")
    other_side(0, "start")
    for k in range(2, line - 1):
        spread_step(k, "start")
        other_side(k - 1, "start")
    for d in range(1, n_tp):
        src = (tp + n_tp - d) % n_tp
        rcopy(stats.at[src], stats.at[src], st_s.at[d], st_r.at[d], sp, partner).wait_recv()
    tot = stats[0]
    for t in range(1, n_tp):
        tot = tot + stats[t]
    tot = jnp.transpose(jnp.concatenate([tot, jnp.zeros((LANES - 8, rows), f32)], axis=0))
    mean = tot[:, 0:1] * (1.0 / (ch * n_tp))
    var = tot[:, 1:2] * (1.0 / (ch * n_tp)) - mean * mean
    y = (conv_out[...] - mean) * lax.rsqrt(var + eps_layer) * cgain[...]
    act[...] = (y * jax.nn.sigmoid(y)).astype(bf16)
    loads["woc"].wait()
    cpart[...] = dot(act[...], v_woc[...])

    for k in range(max(2, line - 1), line):
        spread_step(k, "start")
        other_side(k - 1, "start")
    other_side(line - 1, "start")
    for name in ("wku", "wvu", "sp"):
        loads[name].wait()

    def expand(s, hf):
        lat = kvr[s, hf, 0:half, :]
        start = pl.multiple_of(s * rows + hf * half, half)
        k_all[pl.ds(start, half), :] = dot(lat, v_wku[...]).astype(bf16)
        v_all[pl.ds(start, half), :] = dot(lat, v_wvu[...]).astype(bf16)
        u = dot(kvr[s, hf, half:half + prow, :], v_sp[...]).astype(bf16)
        for g in range(groups):
            r_all[pl.ds(start + g * prow, prow), :] = u[:, g * rw:(g + 1) * rw]

    def expand_all(hf):
        step = 4 if n_sp % 4 == 0 else 1

        def four(i, _):
            for j in range(step):
                expand(i * step + j, hf)
            return 0
        lax.fori_loop(0, n_sp // step, four, 0)

    expand_all(core)
    def relayed(s, _):
        @pl.when(s != sp)
        def _():
            block(s, ky_s, sp, partner, ky_r, 1 - core).wait_recv()
        return 0

    lax.fori_loop(0, n_sp, relayed, 0)
    expand_all(1 - core)

    keys = n_sp * rows
    nk = keys // kchunk
    qb = rows // rblocks
    vw = v_all.shape[1]
    vdim = vw // heads
    scale2 = float((nope + rope) ** -0.5 * np.log2(np.e))
    lane_v = lax.broadcasted_iota(jnp.int32, (qb, vw), 1)

    def attend(b, blk, result):
        hs = range(blk * per, (blk + 1) * per)
        q = jnp.concatenate([qf[h, b * qb:(b + 1) * qb, :] for h in hs], axis=0)

        def scores(at):
            k = jnp.concatenate([k_all[at, blk * LANES:(blk + 1) * LANES], r_all[at, :]], axis=1)
            return dot_t(q, k)

        if nk == 1:
            at = slice(0, keys)
            s = scores(at)
            m = jnp.max(s, axis=1, keepdims=True)
            w = jnp.exp2((s - m) * scale2)
            total = jnp.sum(w, axis=1, keepdims=True)
            o = dot(w.astype(bf16), v_all[at, :])
        else:
            def step(i, carry):
                m, total, o = carry
                at = pl.ds(pl.multiple_of(i * kchunk, kchunk), kchunk)
                s = scores(at)
                nm = jnp.maximum(m, jnp.max(s, axis=1, keepdims=True))
                f = jnp.exp2((m - nm) * scale2)
                w = jnp.exp2((s - nm) * scale2)
                return (nm, total * f + jnp.sum(w, axis=1, keepdims=True),
                        o * f + dot(w.astype(bf16), v_all[at, :]))
            m, total, o = lax.fori_loop(0, nk, step, (
                jnp.full((per * qb, 1), -jnp.inf, f32), jnp.zeros((per * qb, 1), f32),
                jnp.zeros((per * qb, vw), f32)))
        o = o / total
        for i, h in enumerate(hs):
            mask = (lane_v >= h * vdim) & (lane_v < (h + 1) * vdim)
            result = jnp.where(mask, o[i * qb:(i + 1) * qb], result)
        return result

    def partial(b, t, a):
        cols = pl.ds(pl.multiple_of(t * dl, LANES), dl)
        return (dot(a, v_woa[:, cols]) + cpart[b * qb:(b + 1) * qb, cols]).astype(bf16)

    def pcopy(b, j):
        return rcopy(to_partner.at[b, j], from_partner.at[b, j], pp_s.at[b, j], pp_r.at[b, j], sp, partner)

    def ccopy(b, j):
        return rcopy(to_cross.at[b, j], from_cross.at[b, j], cc_s.at[b, j], cc_r.at[b, j],
                     sp, ((pair + j) % pairs) * 2 + core)

    def project(b, a):
        for j in list(range(1, pairs)) + [0]:
            t = ((pair + j) % pairs) * 2
            to_partner[b, j] = partial(b, t + (1 - core), a)
            pcopy(b, j).start()
        for j in range(pairs):
            t = ((pair + j) % pairs) * 2
            own_part[b, j] = partial(b, t + core, a)

    def cross(b):
        for j in range(1, pairs):
            pcopy(b, j).wait_recv()
            to_cross[b, j] = (own_part[b, j].astype(f32) + from_partner[b, j].astype(f32)).astype(bf16)
            ccopy(b, j).start()

    zero = jnp.zeros((qb, vw), f32)
    loads["woa"].wait()
    for b in range(rblocks):
        a = zero
        for blk in range(heads // per):
            a = attend(b, blk, a)
            if b and blk == 0:
                cross(b - 1)
        project(b, a.astype(bf16))
    def done(b):
        return pltpu.make_async_copy(result.at[b], out.at[pl.ds(b * qb, qb)], out_s.at[b])

    cross(rblocks - 1)
    for b in range(rblocks):
        pcopy(b, 0).wait_recv()
        total = own_part[b, 0].astype(f32) + from_partner[b, 0].astype(f32)
        for j in range(1, pairs):
            ccopy(b, j).wait_recv()
            total = total + from_cross[b, j].astype(f32)
        result[b] = total.astype(bf16)
        done(b).start()
    for b in range(rblocks):
        for j in range(pairs):
            pcopy(b, j).wait_send()
        for j in range(1, pairs):
            ccopy(b, j).wait_send()
        done(b).wait()
    for k in range(line):
        spread_step(k, "wait_send")
        other_side(k, "wait_send")
    for c in sends:
        c.wait_send()


def per_device(n_sp, n_tp, *args):
    (tokens, in_gain, query_down, latent_down, rope_down, query_gain, latent_gain, query_nope,
     query_rope, key_up, value_up, conv_value, conv_gate, conv_taps, conv_bias, channel_gain,
     out_attend, out_conv) = args
    rows, dl = tokens.shape
    rope = rope_down.shape[1]
    heads = query_rope.shape[1] // rope
    nope = query_nope.shape[1] // heads
    kvw, qw = latent_down.shape[1], query_down.shape[1]
    ch = conv_value.shape[1]
    groups, half = kvw // rope, rows // 2
    prow = half // groups
    rw = heads * rope
    pairs = n_tp // 2
    tchunks, rblocks = 4, 2
    keys = n_sp * rows
    kchunk = min(keys, 2048)
    qb = rows // rblocks
    pad = -(-(conv_taps.shape[0] // 2) // 16) * 16
    freqs = np.float64(theta) ** (-np.arange(rope // 2) / (rope // 2))
    freqs = np.tile(freqs, 2 * groups)[None, :]
    off = np.arange(rows)[:, None] * freqs
    base = (np.arange(n_sp) * rows)[:, None] * freqs
    tables = [np.cos(off), np.sin(off), np.cos(base), np.sin(base)]
    tables = [jnp.asarray(t.astype(np.float32)) for t in tables]
    l = np.arange(kvw)[:, None]
    m = np.arange(groups * rw)[None, :]
    spread_mat = jnp.asarray(((l // rope == m // rw) & (l % rope == m % rope)).astype(np.float32), bf16)
    row = lambda v: v.reshape(1, -1)
    rope_t = rope_down.T
    ins = (tokens, row(in_gain), query_down, latent_down, rope_t, row(query_gain), row(latent_gain),
           query_nope, query_rope, key_up, value_up, conv_value, conv_gate, conv_taps, row(conv_bias),
           row(channel_gain), out_attend, out_conv, *tables, spread_mat)
    specs = [pl.BlockSpec(memory_space=pltpu.HBM)] * len(ins)
    vm = lambda a: pltpu.VMEM(a.shape, a.dtype)
    D = lambda *s: pltpu.SemaphoreType.DMA(s)
    scratch = [
        pltpu.VMEM((n_tp, rows, dl), bf16), vm(query_down), vm(latent_down), vm(rope_t),
        vm(query_nope), vm(query_rope), vm(key_up), vm(value_up), vm(conv_value), vm(conv_gate),
        vm(out_attend), vm(out_conv), vm(spread_mat),
        *[vm(ins[i]) for i in (1, 5, 6, 13, 14, 15, 18, 19, 20, 21)],
        pltpu.VMEM((rows, qw), f32), pltpu.VMEM((rows, kvw), f32), pltpu.VMEM((rows, rope), f32),
        pltpu.VMEM((rows, ch), f32), pltpu.VMEM((rows, ch), f32),
        pltpu.VMEM((n_sp, 2, half + prow, kvw), bf16),
        pltpu.VMEM((keys, key_up.shape[1]), bf16), pltpu.VMEM((keys, value_up.shape[1]), bf16),
        pltpu.VMEM((keys, rw), bf16), pltpu.VMEM((heads, rows, LANES + rw), bf16),
        pltpu.VMEM((rows + 2 * pad, ch), bf16), pltpu.VMEM((rows + 2 * pad, ch), f32),
        pltpu.VMEM((rows, ch), f32), pltpu.VMEM((n_tp, 8, rows), f32), pltpu.VMEM((rows, ch), bf16),
        pltpu.VMEM((rows, n_tp * dl), f32),
        pltpu.VMEM((rblocks, pairs, qb, dl), bf16), pltpu.VMEM((rblocks, pairs, qb, dl), bf16),
        pltpu.VMEM((rblocks, pairs, qb, dl), bf16), pltpu.VMEM((rblocks, pairs, qb, dl), bf16),
        pltpu.VMEM((rblocks, pairs, qb, dl), bf16),
        pltpu.VMEM((rblocks, qb, dl), bf16),
        D(23), D(pairs, tchunks), D(pairs, tchunks), pltpu.SemaphoreType.DMA, pltpu.SemaphoreType.DMA,
        D(pairs, tchunks), D(pairs, tchunks), *[D(n_sp)] * 6,
        D(2), D(2), D(n_tp), D(n_tp), D(rblocks, pairs), D(rblocks, pairs),
        D(rblocks, pairs), D(rblocks, pairs), D(rblocks),
    ]
    return pl.pallas_call(
        functools.partial(body, n_sp, n_tp, rope, nope, heads, tchunks, rblocks, kchunk),
        out_shape=jax.ShapeDtypeStruct((rows, dl), bf16),
        in_specs=specs,
        out_specs=pl.BlockSpec(memory_space=pltpu.HBM),
        scratch_shapes=scratch,
        compiler_params=pltpu.CompilerParams(
            collective_id=0, has_side_effects=True, vmem_limit_bytes=60 << 20),
        name="layer",
    )(*ins)


def solution(mesh):
    in_specs = (
        P("sp", "tp"), P(), P(), P(), P(), P(), P(), P(None, "tp"), P(None, "tp"), P(None, "tp"),
        P(None, "tp"), P(None, "tp"), P(None, "tp"), P(None, "tp"), P("tp"), P("tp"),
        P("tp", None), P("tp", None),
    )
    return jax.shard_map(
        functools.partial(per_device, mesh.shape["sp"], mesh.shape["tp"]),
        mesh=mesh, in_specs=in_specs, out_specs=P("sp", "tp"), check_vma=False)
```
